32 devices in a mesh: ep: 8 (over z, y), tp: 4 (over x, core).
Axes of the slice: x: 2, y: 2, z: 4, core: 2. Of those that a mesh axis runs over, the one named last changes fastest.
Arguments:
- conv_value: bfloat16 [12288, 2048], P(('ep', 'tp')), may hold values from -6 to 6
- conv_gate: bfloat16 [12288, 2048], P(('ep', 'tp')), may hold values from -6 to 6
- conv_taps: float32 [31, 2048], replicated, may hold values from -1 to 1
- conv_gain: float32 [2048], replicated, may hold values from 0.1 to 1.9
- conv_bias: float32 [2048], replicated, may hold values from -3 to 3
- conv_projection: bfloat16 [2048, 4096], P(None, 'tp'), may hold values from -0.125 to 0.125
- expert_input: bfloat16 [4096, 4096], P('ep'), may hold values from -6 to 6
- expert_gain: float32 [4096], replicated, may hold values from 0.1 to 1.9
- route_experts: int32 [4096, 2], P('ep'), may hold values from 0 to 31, all different within a row; in each aligned block of 128 rows (0 to 127, 128 to 255, ...) at most 16 rows name the same one
- group_gate: float32 [4096], P('ep'), may hold values from 0.3 to 1
- expert_gate: float32 [4096, 2], P('ep'), may hold values from 0.1 to 1
- gate_weight: bfloat16 [32, 4096, 1024], P('ep', None, 'tp'), may hold values from -0.09375 to 0.09375
- up_weight: bfloat16 [32, 4096, 1024], P('ep', None, 'tp'), may hold values from -0.09375 to 0.09375
- down_weight: bfloat16 [32, 1024, 4096], P('ep', None, 'tp'), may hold values from -0.1875 to 0.1875
Outputs:
- conv_out: bfloat16 [12288, 4096], P('ep', 'tp')
- expert_out: bfloat16 [4096, 4096], P('ep', 'tp')
The draws below stay inside these ranges and needn't reach their ends.
Inputs may be any that keep to these rules, and one draw needn't show every extreme that they name: `route_experts`: each row names 2 different experts; in each aligned block of 128 rows no expert is named more than 16 times, and in some blocks one expert is named exactly 16 times.
All inputs are finite; a program needn't handle non-finite values.
Results may differ from the reference program's by a relative error of at most 0.0071.
Values may be sent and summed in bfloat16 or wider, within the bound.
A program may use at most 128 MiB of HBM per device.

```python
import math
import jax
import jax.numpy as jnp
import numpy as np
from jax import lax

D = 4096
CONV = 2048
KERNEL = 31
HID = 1024
EXPERTS = 32
TOP = 2
MOE_DEV = 128
CAP = 16
SEQ = 12288
MOE_ROWS = 4096


def level_of(stream_key, shape, split, low, largest):
    level = 1.0
    for position, blocks in split:
        draws = jax.random.uniform(jax.random.fold_in(jax.random.fold_in(stream_key, 6), position), (blocks,), jnp.float32, low / len(split), largest / len(split))
        level = level * jnp.repeat(jnp.exp(draws), shape[position] // blocks).reshape((-1,) + (1,) * (len(shape) - 1 - position))
    return level


def assign_block(stream_key, own, number, rows, number_of, top, limit, slope):
    sequence = jax.random.permutation(stream_key, number_of)
    crowded, common = portions_of(number_of, rows * top, limit, slope, True), portions_of(number_of, rows * top, limit, slope, False)
    places = jnp.arange(number_of)

    def named(tallies, offset_by):
        used = int((tallies > 0).sum())
        fixed = max(1, used // 4)
        passed = fixed + (places - fixed + offset_by * (used - fixed)) % max(1, number_of - fixed)
        return jnp.zeros((number_of,), jnp.int32).at[sequence[jnp.where(places < fixed, places, passed)]].set(jnp.asarray(tallies, jnp.int32))

    tallies = jnp.where(number % 4 == 0, named(crowded, number // 4), named(common, number - number // 4 - 1))
    mixed = jax.random.permutation(jax.random.fold_in(own, 3), number_of)
    donor, sink = mixed[0:number_of // 2 * 2:2], mixed[1:number_of // 2 * 2:2]
    margin = jnp.minimum(tallies[donor] - 1, limit - tallies[sink]) // 2
    margin = jnp.where((donor == sequence[0]) | (sink == sequence[0]) | (tallies[sink] == 0), 0, jnp.maximum(margin, 0))
    passed = jax.random.randint(jax.random.fold_in(own, 4), (number_of // 2,), 0, 1 << 20) % (margin + 1)
    tallies = tallies.at[donor].add(-passed).at[sink].add(passed)
    items = jnp.searchsorted(jnp.cumsum(tallies), jnp.arange(rows * top), side="right").astype(jnp.int32)
    table = items.reshape(top, rows).T
    table = table[jax.random.permutation(jax.random.fold_in(own, 1), rows)]
    offset_by = jax.random.randint(jax.random.fold_in(own, 2), (rows, 1), 0, top)
    return jnp.take_along_axis(table, (jnp.arange(top)[None, :] + offset_by) % top, axis=1)


def portions_of(count, total, bound, lean, full):
    weights = [(1 << 20) // math.isqrt(grade ** lean) + 1 for grade in range(1, count + 1)]
    largest = bound if full else min(bound, max(-(-total // count), total * weights[0] // sum(weights)))
    least = 1 if total - largest >= count - 1 else 0
    holding, rest = [largest] + [least] * (count - 1), total - largest - least * (count - 1)
    while rest > 0:
        candidates = [i for i in range(1, count) if holding[i] < largest] or [i for i in range(1, count) if holding[i] < bound]
        whole, remaining = sum([weights[i] for i in candidates]), rest
        for i in candidates:
            more = min(bound - holding[i], max(1, remaining * weights[i] // whole), rest)
            holding[i] = holding[i] + more
            rest = rest - more
    return np.array(holding)


def normal_values(rng, shape, deviation, most, shards=(), kind=jnp.bfloat16):
    level = level_of(rng, shape, shards, -0.22, 0.18) if shards else 1.0
    values = jax.random.normal(rng, shape, jnp.float32) * deviation * level
    return jnp.minimum(jnp.maximum(values, -most), most).astype(kind)


def setup_inputs(seed: int = 0) -> dict:
    splits = jax.random.split(jax.random.key(seed), 15)
    conv_value = normal_values(splits[0], (SEQ, CONV), 1.0, 6.0, ((0, 32),))
    conv_gate = normal_values(splits[1], (SEQ, CONV), 1.0, 6.0, ((0, 32),))
    conv_taps = normal_values(splits[2], (KERNEL, CONV), KERNEL ** -0.5, 1.0, (), jnp.float32)
    conv_gain = jnp.clip(1.0 + 0.18 * jax.random.normal(splits[3], (CONV,), jnp.float32), 0.1, 1.9)
    conv_bias = normal_values(splits[4], (CONV,), 0.5, 3.0, (), jnp.float32)
    conv_projection = normal_values(splits[5], (CONV, D), CONV ** -0.5, 0.125, ((1, 4),))
    expert_input = normal_values(splits[6], (MOE_ROWS, D), 1.0, 6.0, ((0, 8),))
    expert_gain = jnp.clip(1.0 + 0.18 * jax.random.normal(splits[7], (D,), jnp.float32), 0.1, 1.9)
    route_experts_keys = jax.random.split(jax.random.fold_in(splits[8], 1), MOE_ROWS // MOE_DEV)
    route_experts_turns = jax.random.permutation(jax.random.fold_in(splits[8], 3), MOE_ROWS // MOE_DEV)
    route_experts = jax.vmap(lambda own, number: assign_block(jax.random.fold_in(splits[8], 2), own, number, MOE_DEV, EXPERTS, TOP, CAP, 2))(route_experts_keys, route_experts_turns).reshape((MOE_ROWS, TOP))
    group_gate = jnp.clip(0.3 + 0.7 * jax.random.uniform(splits[9], (MOE_ROWS,), jnp.float32) ** level_of(splits[9], (MOE_ROWS,), ((0, 8),), -0.2, 0.2), 0.3, 1.0)
    expert_gate = jnp.clip(jnp.exp(math.log(1.0) - 2.3025851 * jax.random.uniform(splits[10], (MOE_ROWS, TOP), jnp.float32) ** level_of(splits[10], (MOE_ROWS, TOP), ((0, 8),), -0.2, 0.2)), 0.1, 1.0)
    gate_weight = normal_values(splits[11], (EXPERTS, D, HID), D ** -0.5, 0.09375, ((0, 8), (2, 4)))
    up_weight = normal_values(splits[12], (EXPERTS, D, HID), D ** -0.5, 0.09375, ((0, 8), (2, 4)))
    down_weight = normal_values(splits[13], (EXPERTS, HID, D), HID ** -0.5, 0.1875, ((0, 8), (2, 4)))
    return dict(conv_value=conv_value, conv_gate=conv_gate, conv_taps=conv_taps, conv_gain=conv_gain, conv_bias=conv_bias, conv_projection=conv_projection, expert_input=expert_input, expert_gain=expert_gain, route_experts=route_experts, group_gate=group_gate, expert_gate=expert_gate, gate_weight=gate_weight, up_weight=up_weight, down_weight=down_weight)


epsilon = 1e-06

def root_mean_norm(values, gain):
    widened = values.astype(jnp.float32)
    inverse_rms = lax.rsqrt(lax.optimization_barrier(jnp.mean(widened * widened, axis=-1, keepdims=True)) + epsilon)
    return (widened * inverse_rms * gain).astype(jnp.bfloat16)

def reference(conv_value, conv_gate, conv_taps, conv_gain, conv_bias, conv_projection, expert_input, expert_gain, route_experts, group_gate, expert_gate, gate_weight, up_weight, down_weight):
    gated_rows = (conv_value.astype(jnp.float32) * jax.nn.sigmoid(conv_gate.astype(jnp.float32))).astype(jnp.bfloat16)
    reach_back = KERNEL - 1
    extended = jnp.concatenate([jnp.zeros((reach_back, CONV), jnp.bfloat16), gated_rows], axis=0)
    mixed_conv = jnp.zeros((SEQ, CONV), jnp.float32)
    for lag_step in range(KERNEL):
        window = lax.slice_in_dim(extended, reach_back - lag_step, reach_back - lag_step + SEQ, axis=0)
        mixed_conv = mixed_conv + conv_taps[lag_step] * window.astype(jnp.float32)
    center = mixed_conv - lax.optimization_barrier(jnp.mean(mixed_conv, axis=-1, keepdims=True))
    spread = lax.optimization_barrier(jnp.mean(center * center, axis=-1, keepdims=True))
    activated = jax.nn.silu(center * lax.rsqrt(spread + epsilon) * conv_gain + conv_bias).astype(jnp.bfloat16)
    conv_out = jnp.dot(activated, conv_projection, preferred_element_type=jnp.float32).astype(jnp.bfloat16)
    normed = root_mean_norm(expert_input, expert_gain)
    blocks = MOE_ROWS // MOE_DEV
    picked_experts = route_experts.reshape(blocks, MOE_DEV * TOP)
    onehot = (picked_experts[:, :, None] == jnp.arange(EXPERTS, dtype=jnp.int32)[None, None, :]).astype(jnp.int32)
    before = jnp.cumsum(onehot, axis=1) - onehot
    positions = lax.optimization_barrier(jnp.sum(before * onehot, axis=2)).astype(jnp.int32)
    block_index = jnp.arange(blocks, dtype=jnp.int32)[:, None]
    token_index = block_index * MOE_DEV + jnp.arange(MOE_DEV * TOP, dtype=jnp.int32)[None, :] // TOP
    column = block_index * CAP + positions
    route_share = group_gate[:, None] * expert_gate / lax.optimization_barrier(jnp.sum(expert_gate, axis=1, keepdims=True))
    route_share = route_share.reshape(blocks, MOE_DEV * TOP)
    source = jnp.full((EXPERTS, blocks * CAP), -1, jnp.int32).at[picked_experts, column].set(token_index)
    shares = jnp.zeros((EXPERTS, blocks * CAP), jnp.float32).at[picked_experts, column].set(route_share)

    def one_expert(running, packed):
        indices, slot_shares, gate_matrix, up_matrix, down_matrix = packed
        safe_index = jnp.maximum(indices, 0)
        taken_rows = jnp.take(normed, safe_index, axis=0)
        gate_part = jnp.dot(taken_rows, gate_matrix, preferred_element_type=jnp.float32)
        up_part = jnp.dot(taken_rows, up_matrix, preferred_element_type=jnp.float32)
        hidden = (jax.nn.silu(gate_part) * up_part).astype(jnp.bfloat16)
        result = jnp.dot(hidden, down_matrix, preferred_element_type=jnp.float32).astype(jnp.bfloat16)
        return (running.at[safe_index].add(slot_shares[:, None] * result.astype(jnp.float32)), None)
    running, _ = lax.scan(one_expert, jnp.zeros((MOE_ROWS, D), jnp.float32), (source, shares, gate_weight, up_weight, down_weight))
    return (conv_out, running.astype(jnp.bfloat16))
```

```python
import functools

import jax
import jax.numpy as jnp
from jax import lax
from jax.experimental import pallas as pl
from jax.experimental.pallas import tpu as pltpu
from jax.sharding import PartitionSpec as P

EXPERTS = 32
TOP = 2
MOE_DEV = 128
CAP = 16

MESH = pl.DeviceIdType.MESH

LANES = 128
CONV_CHUNKS = 4
EARLY_CHUNKS = 2

epsilon = 1e-06


def slot_numbers(route_experts):
    picked = route_experts.reshape(-1, MOE_DEV * TOP)
    onehot = (picked[:, :, None] == jnp.arange(EXPERTS, dtype=jnp.int32)).astype(jnp.bfloat16)
    order = jnp.arange(MOE_DEV * TOP, dtype=jnp.int32)
    earlier = (order[:, None] > order[None, :]).astype(jnp.bfloat16)
    before = jnp.einsum("ij,bje->bie", earlier, onehot, preferred_element_type=jnp.float32)
    positions = jnp.sum(before * onehot.astype(jnp.float32), axis=2).astype(jnp.int32)
    return (picked * CAP + positions).reshape(-1, MOE_DEV, TOP)


def on_line(place, order, length):
    upper = 2 * place // length
    short = place + upper * (length - 1 - 2 * place)
    beyond = (order - 2 * short - 1 + length) // length
    both = place + (1 - 2 * (order % 2)) * ((order + 1) // 2)
    single = place + (1 - 2 * upper) * (order - short)
    return both + beyond * (single - both)


def fused_kernel(
    count,
    reach,
    tokens_hbm,
    expert_gain,
    routes,
    gate_hbm,
    up_hbm,
    down_hbm,
    value_hbm,
    switch_hbm,
    taps,
    conv_gain,
    conv_bias,
    returned,
    gathered,
    blocks,
    block_routes,
    spare,
    normed,
    crossing,
    landed,
    gate,
    up,
    down,
    hidden,
    result,
    value,
    switch,
    halo,
    gated,
    mixed,
    active,
    load_sem,
    conv_load,
    halo_send,
    halo_recv,
    route_send,
    route_recv,
    hop_send,
    hop_recv,
    cross_send,
    cross_recv,
    side_send,
    side_recv,
    near_send,
    near_recv,
    unit_send,
    unit_recv,
    back_send,
    back_recv,
    conv_kept,
    conv_send,
    conv_recv,
):
    group, quarter = lax.axis_index("ep"), lax.axis_index("tp")
    quarters = landed.shape[1]
    near, side = quarter + 1 - 2 * (quarter % 2), (quarter + 2) % 4
    length = count // 2
    place, across = group // 2, group % 2
    other = place * 2 + 1 - across
    local = gate.shape[0]
    size = landed.shape[2]
    width = landed.shape[3]
    rows_per = value.shape[1]
    border = halo.shape[1]
    total = count * quarters
    flat = group * quarters + quarter
    after, before = (flat + 1) % total, (flat + total - 1) % total

    loads = [
        pltpu.make_async_copy(source, target, load_sem.at[number])
        for number, (source, target) in enumerate(
            [
                (tokens_hbm.at[pl.ds(quarter * MOE_DEV, MOE_DEV)], blocks.at[place]),
                (gate_hbm, gate),
                (up_hbm, up),
                (down_hbm, down),
            ]
        )
    ]
    loads[0].start()

    barrier = pltpu.get_barrier_semaphore()

    def greet(m, carry):
        pl.semaphore_signal(
            barrier, inc=1, device_id=((group + m) % count, quarter), device_id_type=MESH
        )
        return carry

    lax.fori_loop(1, count, greet, 0)
    for member in (near, side):
        pl.semaphore_signal(barrier, inc=1, device_id=(group, member), device_id_type=MESH)
    for member in (after, before):
        pl.semaphore_signal(
            barrier,
            inc=1,
            device_id=(member // quarters, member % quarters),
            device_id_type=MESH,
        )

    def conv_loads(c):
        rows = pl.ds(c * rows_per, rows_per)
        return [
            pltpu.make_async_copy(source.at[rows], target.at[c % 2], conv_load.at[number, c % 2])
            for number, (source, target) in enumerate([(value_hbm, value), (switch_hbm, switch)])
        ]

    for load in conv_loads(0):
        load.start()
    pl.semaphore_wait(barrier, count + 3)

    def copy(source, target, send, recv, device):
        return pltpu.make_async_remote_copy(
            src_ref=source,
            dst_ref=target,
            send_sem=send,
            recv_sem=recv,
            device_id=device,
            device_id_type=MESH,
        )

    def hop(origin, way):
        device = ((place + 1 - 2 * way) * 2 + across, quarter)
        spot = blocks.at[origin]
        return copy(spot, spot, hop_send.at[origin, way], hop_recv.at[origin], device)

    def route(m):
        device = ((place + m) % length * 2 + across, quarter)
        spot = block_routes.at[place]
        return copy(routes.at[quarter], spot, route_send.at[m], route_recv.at[place], device)

    def route_from(origin):
        spot = block_routes.at[origin]
        return copy(
            routes.at[quarter], spot, route_send.at[0], route_recv.at[origin], (other, quarter)
        )

    def edge(number):
        source = (value_hbm, switch_hbm)[number]
        last = source.at[pl.ds(source.shape[0] - border, border)]
        device = (after // quarters, after % quarters)
        return copy(last, halo.at[number], halo_send.at[number], halo_recv.at[number], device)

    def cross(order):
        spot = landed.at[2 * order + 1, quarter]
        send, recv = cross_send.at[order], cross_recv.at[order]
        return copy(crossing.at[order], spot, send, recv, (other, quarter))

    def to_side(m):
        spot = landed.at[m, quarter]
        return copy(spot, spot, side_send.at[m], side_recv.at[m], (group, side))

    def to_near(m, number):
        spot = landed.at[m, (quarter, side)[number]]
        send, recv = near_send.at[m, number], near_recv.at[m, number]
        return copy(spot, spot, send, recv, (group, near))

    def units(p, number):
        spot = hidden.at[p, (quarter, quarter, side)[number]]
        send, recv = unit_send.at[p, number], unit_recv.at[p, number]
        return copy(spot, spot, send, recv, (group, (side, near, near)[number]))

    def back(m):
        home = on_line(place, m // 2, length) * 2 + (across + m) % 2
        spot = returned.at[group]
        return copy(result.at[m], spot, back_send.at[m], back_recv.at[group], (home, quarter))

    def back_from(origin):
        spot = returned.at[origin]
        return copy(result.at[0], spot, back_send.at[0], back_recv.at[origin], (origin, quarter))

    def kept():
        return pltpu.make_async_copy(result.at[0], returned.at[group], load_sem.at[5])

    def conv_share(c, number):
        rows = pl.ds(c * rows_per, rows_per)
        spot = gathered.at[(quarter, quarter, side)[number], rows]
        source = (active.at[c], active.at[c], spot)[number]
        send, recv = conv_send.at[c, number], conv_recv.at[c, number]
        return copy(source, spot, send, recv, (group, (side, near, near)[number]))

    def conv_keep(c):
        spot = gathered.at[quarter, pl.ds(c * rows_per, rows_per)]
        return pltpu.make_async_copy(active.at[c], spot, conv_kept.at[c])

    loads[0].wait()

    @pl.when(place < length - 1)
    def _():
        hop(place, 0).start()

    @pl.when(place > 0)
    def _():
        hop(place, 1).start()

    def start_route(m, carry):
        route(m).start()
        return carry

    lax.fori_loop(1, length, start_route, 0)
    edge(0).start()
    edge(1).start()
    for load in loads[1:]:
        load.start()

    def normalize(source):
        def some_rows(q, carry):
            rows = pl.ds(pl.multiple_of(q * 16, 16), 16)
            widened = source[rows, :].astype(jnp.float32)
            inverse_rms = lax.rsqrt(jnp.mean(widened * widened, axis=-1, keepdims=True) + epsilon)
            normed[rows, :] = (widened * inverse_rms * expert_gain[...]).astype(jnp.bfloat16)
            return carry

        lax.fori_loop(0, MOE_DEV // 16, some_rows, 0)

    def chosen(table):
        slot = lax.broadcasted_iota(jnp.int32, (2 * size, MOE_DEV), 0)
        second = (slot >= size).astype(jnp.int32)
        within = slot - second * size
        number = (group + second * (other - group)) * local + lax.shift_right_logical(
            within, CAP.bit_length() - 1
        )
        named = (table[0:1, :] == number) | (table[1:2, :] == number)
        row = lax.broadcasted_iota(jnp.int32, (MOE_DEV, MOE_DEV), 0)
        column = lax.broadcasted_iota(jnp.int32, (MOE_DEV, MOE_DEV), 1)
        earlier = jnp.where(row < column, 1.0, 0.0).astype(jnp.bfloat16)
        ones = jnp.where(named, 1.0, 0.0)
        taken = jnp.dot(ones.astype(jnp.bfloat16), earlier, preferred_element_type=jnp.float32)
        wanted = (within & (CAP - 1)).astype(jnp.float32)
        return jnp.where(taken == wanted, ones, 0.0).astype(jnp.bfloat16)

    def fill(table, spot, order, own_only):
        picks = chosen(table)
        piece = 1024

        def some_columns(q, carry):
            columns = pl.ds(pl.multiple_of(q * piece, piece), piece)
            part = jnp.dot(picks, normed[:, columns], preferred_element_type=jnp.float32)
            part = part.astype(jnp.bfloat16)
            landed[spot[0], spot[1], :, columns] = part[:size]

            @pl.when(own_only == 0)
            def _():
                crossing[order, :, columns] = part[size:]

            return carry

        lax.fori_loop(0, width // piece, some_columns, 0)

    def own_block(k, carry):
        member = (quarter + k) % quarters

        @pl.when(k == 0)
        def _():
            normalize(blocks.at[place])

        @pl.when(k > 0)
        def _():
            rows = pl.ds(member * MOE_DEV, MOE_DEV)
            load = pltpu.make_async_copy(tokens_hbm.at[rows], spare, load_sem.at[4])
            load.start()
            load.wait()
            normalize(spare)

        fill(routes.at[member], (0, member), 0, k)

        @pl.when(k == 0)
        def _():
            cross(0).start()

        return carry

    lax.fori_loop(0, quarters, own_block, 0)

    def conv_chunk(c):
        pieces = gated.shape[0]
        slot = c % 2

        @pl.when(c == 0)
        def _():
            edge(0).wait_recv()
            edge(1).wait_recv()

            def first_rows(q, carry):
                lanes = pl.ds(pl.multiple_of(q * LANES, LANES), LANES)
                left = halo[0, :, lanes].astype(jnp.float32)
                right = jax.nn.sigmoid(halo[1, :, lanes].astype(jnp.float32))
                product = (left * right).astype(jnp.bfloat16).astype(jnp.float32)
                gated[q, 0:border, :] = jnp.where(flat == 0, 0.0, product)
                return carry

            lax.fori_loop(0, pieces, first_rows, 0)

        @pl.when(c > 0)
        def _():
            def last_rows(q, carry):
                gated[q, 0:border, :] = gated[q, rows_per : rows_per + border, :]
                return carry

            lax.fori_loop(0, pieces, last_rows, 0)

        for load in conv_loads(c):
            load.wait()

        @pl.when(c + 1 < CONV_CHUNKS)
        def _():
            for load in conv_loads(c + 1):
                load.start()

        def mix(q, sums):
            lanes = pl.ds(pl.multiple_of(q * LANES, LANES), LANES)
            left = value[slot, :, lanes].astype(jnp.float32)
            right = jax.nn.sigmoid(switch[slot, :, lanes].astype(jnp.float32))
            gated[q, border : border + rows_per, :] = (
                (left * right).astype(jnp.bfloat16).astype(jnp.float32)
            )
            amount = jnp.zeros((rows_per, LANES), jnp.float32)
            for tap in range(reach + 1):
                window = gated[q, border - tap : border - tap + rows_per, :]
                amount = amount + taps[tap : tap + 1, lanes] * window
            mixed[q] = amount
            return sums + amount

        sums = lax.fori_loop(0, pieces, mix, jnp.zeros((rows_per, LANES), jnp.float32))
        channels = pieces * LANES
        mean = jnp.sum(sums, axis=-1, keepdims=True) / channels

        def spread_of(q, squares):
            center = mixed[q] - mean
            return squares + center * center

        squares = lax.fori_loop(0, pieces, spread_of, jnp.zeros((rows_per, LANES), jnp.float32))
        spread = jnp.sum(squares, axis=-1, keepdims=True) / channels
        scale = lax.rsqrt(spread + epsilon)

        def activate(q, carry):
            lanes = pl.ds(pl.multiple_of(q * LANES, LANES), LANES)
            level = (mixed[q] - mean) * scale * conv_gain[:, lanes] + conv_bias[:, lanes]
            active[c, :, lanes] = (level * jax.nn.sigmoid(level)).astype(jnp.bfloat16)
            return carry

        lax.fori_loop(0, pieces, activate, 0)
        conv_share(c, 0).start()
        conv_share(c, 1).start()
        conv_keep(c).start()

    def early(c, carry):
        conv_chunk(c)
        return carry

    lax.fori_loop(0, EARLY_CHUNKS, early, 0)

    def to_hidden(p):
        for e in range(local):
            rows = landed[p, :, e * CAP : (e + 1) * CAP, :]
            rows = rows.reshape(rows.shape[0] * CAP, rows.shape[2])
            gate_part = jnp.dot(rows, gate[e], preferred_element_type=jnp.float32)
            up_part = jnp.dot(rows, up[e], preferred_element_type=jnp.float32)
            part = (gate_part / (1.0 + jnp.exp(-gate_part)) * up_part).astype(jnp.bfloat16)
            part = part.reshape(-1, CAP, part.shape[1])
            hidden[p, quarter, :, e * CAP : (e + 1) * CAP, :] = part

    def to_result(p):
        for e in range(local):
            parts = [hidden[p, t, :, e * CAP : (e + 1) * CAP, :] for t in range(hidden.shape[1])]
            parts = [part.reshape(-1, part.shape[2]) for part in parts]
            total = jnp.dot(
                jnp.concatenate(parts, axis=1), down[e], preferred_element_type=jnp.float32
            )
            total = total.astype(jnp.bfloat16).reshape(-1, CAP, total.shape[1])
            result[p, :, e * CAP : (e + 1) * CAP, :] = total

    loads[1].wait()
    loads[2].wait()
    loads[3].wait()

    def step(j, carry):
        @pl.when((j >= 3) & (j < count + 3))
        def _():
            units(j - 3, 0).wait_recv()
            units(j - 3, 2).start()

        @pl.when((j >= 2) & (j < count) & (j % 2 == 0))
        def _():
            order = j // 2
            origin = on_line(place, order, length)
            hop(origin, 0).wait_recv()

            @pl.when((origin < place) & (place < length - 1))
            def _():
                hop(origin, 0).start()

            @pl.when((origin > place) & (place > 0))
            def _():
                hop(origin, 1).start()

            normalize(blocks.at[origin])
            route_from(origin).wait_recv()
            fill(block_routes.at[origin], (j, quarter), order, 0)
            cross(order).start()

        @pl.when((j >= 1) & (j < count) & (j % 2 == 1))
        def _():
            cross(j // 2).wait_recv()

        @pl.when((j >= 1) & (j < count))
        def _():
            to_side(j).start()
            to_near(j, 0).start()

        @pl.when((j >= 3) & (j < count + 3))
        def _():
            units(j - 3, 1).wait_recv()
            units(j - 3, 2).wait_recv()
            to_result(j - 3)

        @pl.when((j >= 2) & (j < count + 1))
        def _():
            to_side(j - 1).wait_recv()
            to_near(j - 1, 1).start()

        @pl.when((j >= 3) & (j < count + 2))
        def _():
            to_near(j - 2, 0).wait_recv()
            to_near(j - 2, 1).wait_recv()

        @pl.when((j >= 2) & (j < count + 2))
        def _():
            to_hidden(j - 2)

        @pl.when((j >= 2) & (j < 2 + CONV_CHUNKS - EARLY_CHUNKS))
        def _():
            conv_chunk(j - 2 + EARLY_CHUNKS)

        @pl.when(j == 3)
        def _():
            kept().start()

        @pl.when((j >= 4) & (j < count + 3))
        def _():
            back(j - 3).start()

        @pl.when((j >= 2) & (j < count + 2))
        def _():
            units(j - 2, 0).start()
            units(j - 2, 1).start()

        @pl.when((j >= count) & (j < count + 1))
        def _():
            for c in range(CONV_CHUNKS):
                conv_share(c, 0).wait_recv()
                conv_share(c, 2).start()

        return carry

    lax.fori_loop(1, count + 3, step, 0)

    @pl.when(place < length - 1)
    def _():
        hop(place, 0).wait_send()

    @pl.when(place > 0)
    def _():
        hop(place, 1).wait_send()

    def finish_line(m, carry):
        route(m).wait_send()
        origin = on_line(place, m, length)

        @pl.when((origin < place) & (place < length - 1))
        def _():
            hop(origin, 0).wait_send()

        @pl.when((origin > place) & (place > 0))
        def _():
            hop(origin, 1).wait_send()

        cross(m).wait_send()
        return carry

    cross(0).wait_send()
    lax.fori_loop(1, length, finish_line, 0)
    edge(0).wait_send()
    edge(1).wait_send()

    for c in range(CONV_CHUNKS):
        conv_keep(c).wait()
        for number in range(3):
            conv_share(c, number).wait_send()
        conv_share(c, 1).wait_recv()
        conv_share(c, 2).wait_recv()

    def finish_units(p, carry):
        for number in range(3):
            units(p, number).wait_send()
        return carry

    lax.fori_loop(0, count, finish_units, 0)

    def finish(m, carry):
        to_side(m).wait_send()
        to_near(m, 0).wait_send()
        to_near(m, 1).wait_send()
        back(m).wait_send()
        back_from((group + m) % count).wait_recv()
        return carry

    lax.fori_loop(1, count, finish, 0)
    kept().wait()


def fused(
    tokens,
    expert_gain,
    routes,
    gate_weight,
    up_weight,
    down_weight,
    conv_value,
    conv_gate,
    conv_taps,
    conv_gain,
    conv_bias,
    count,
):
    width = tokens.shape[1]
    quarters = tokens.shape[0] // MOE_DEV
    local, units, features = gate_weight.shape[0], gate_weight.shape[2], down_weight.shape[2]
    size = local * CAP
    length = count // 2
    positions, channels = conv_value.shape
    rows_per = positions // CONV_CHUNKS
    reach = conv_taps.shape[0] - 1
    border = -(-reach // 16) * 16
    rows = count * quarters * size
    dma = pltpu.SemaphoreType.DMA
    anywhere = pl.BlockSpec(memory_space=pl.ANY)
    inside = pl.BlockSpec(memory_space=pltpu.VMEM)
    return pl.pallas_call(
        functools.partial(fused_kernel, count, reach),
        out_shape=(
            jax.ShapeDtypeStruct((count, quarters, size, features), jnp.bfloat16),
            jax.ShapeDtypeStruct((quarters, positions, channels), jnp.bfloat16),
        ),
        in_specs=[
            anywhere,
            inside,
            inside,
            anywhere,
            anywhere,
            anywhere,
            anywhere,
            anywhere,
            inside,
            inside,
            inside,
        ],
        out_specs=(anywhere, anywhere),
        scratch_shapes=[
            pltpu.VMEM((length, MOE_DEV, width), jnp.bfloat16),
            pltpu.VMEM((length,) + routes.shape[1:], jnp.int32),
            pltpu.VMEM((MOE_DEV, width), jnp.bfloat16),
            pltpu.VMEM((MOE_DEV, width), jnp.bfloat16),
            pltpu.VMEM((length, size, width), jnp.bfloat16),
            pltpu.VMEM((count, quarters, size, width), jnp.bfloat16),
            pltpu.VMEM(gate_weight.shape, jnp.bfloat16),
            pltpu.VMEM(up_weight.shape, jnp.bfloat16),
            pltpu.VMEM(down_weight.shape, jnp.bfloat16),
            pltpu.VMEM((count, quarters, quarters, size, units), jnp.bfloat16),
            pltpu.VMEM((count, quarters, size, features), jnp.bfloat16),
            pltpu.VMEM((2, rows_per, channels), jnp.bfloat16),
            pltpu.VMEM((2, rows_per, channels), jnp.bfloat16),
            pltpu.VMEM((2, border, channels), jnp.bfloat16),
            pltpu.VMEM((channels // LANES, border + rows_per, LANES), jnp.float32),
            pltpu.VMEM((channels // LANES, rows_per, LANES), jnp.float32),
            pltpu.VMEM((CONV_CHUNKS, rows_per, channels), jnp.bfloat16),
            dma((6,)),
            dma((2, 2)),
            dma((2,)),
            dma((2,)),
            dma((length,)),
            dma((length,)),
            dma((length, 2)),
            dma((length,)),
            dma((length,)),
            dma((length,)),
            dma((count,)),
            dma((count,)),
            dma((count, 2)),
            dma((count, 2)),
            dma((count, 3)),
            dma((count, 3)),
            dma((count,)),
            dma((count,)),
            dma((CONV_CHUNKS,)),
            dma((CONV_CHUNKS, 3)),
            dma((CONV_CHUNKS, 3)),
        ],
        compiler_params=pltpu.CompilerParams(
            collective_id=0, has_side_effects=True, vmem_limit_bytes=67_043_328
        ),
        cost_estimate=pl.CostEstimate(
            flops=40 * rows * width * units, bytes_accessed=250_000_000, transcendentals=0
        ),
    )(
        tokens,
        expert_gain,
        routes,
        gate_weight,
        up_weight,
        down_weight,
        conv_value,
        conv_gate,
        conv_taps,
        conv_gain,
        conv_bias,
    )


def weighed(results, slots, share):
    wanted = jnp.arange(results.shape[0] * results.shape[2], dtype=jnp.int32)
    same = slots[:, :, :, None] == wanted[None, None, None, :]
    weights = jnp.sum(jnp.where(same, share[:, :, :, None], 0.0), axis=2)
    high = weights.astype(jnp.bfloat16)
    low = (weights - high.astype(jnp.float32)).astype(jnp.bfloat16)
    both = jnp.concatenate([high, low], axis=1)
    both = both.reshape(both.shape[:2] + (results.shape[0], results.shape[2]))
    total = jnp.einsum("qrks,kqsd->qrd", both, results, preferred_element_type=jnp.float32)
    return total[:, : total.shape[1] // 2] + total[:, total.shape[1] // 2 :]


def on_device(
    conv_value,
    conv_gate,
    conv_taps,
    conv_gain,
    conv_bias,
    conv_projection,
    expert_input,
    expert_gain,
    route_experts,
    group_gate,
    expert_gate,
    gate_weight,
    up_weight,
    down_weight,
):
    count = lax.axis_size("ep")
    slots = slot_numbers(route_experts)
    quarters = slots.shape[0]
    share = group_gate[:, None] * expert_gate / jnp.sum(expert_gate, axis=1, keepdims=True)
    share = share.reshape(slots.shape)
    routes = jnp.swapaxes(route_experts.reshape(quarters, MOE_DEV, TOP), 1, 2)
    routes = jnp.pad(routes, ((0, 0), (0, 8 - TOP), (0, 0)))
    results, gathered = fused(
        expert_input,
        expert_gain[None],
        routes,
        gate_weight,
        up_weight,
        down_weight,
        conv_value,
        conv_gate,
        conv_taps,
        conv_gain[None],
        conv_bias[None],
        count,
    )
    total = weighed(results, slots, share)
    expert_out = total.reshape(quarters * MOE_DEV, -1).astype(jnp.bfloat16)
    conv_out = jnp.dot(
        gathered.reshape(-1, gathered.shape[2]),
        conv_projection,
        preferred_element_type=jnp.float32,
    ).astype(jnp.bfloat16)
    return (conv_out, expert_out)


def solution(mesh):
    return jax.shard_map(
        on_device,
        mesh=mesh,
        in_specs=(
            P(("ep", "tp"), None),
            P(("ep", "tp"), None),
            P(),
            P(),
            P(),
            P(None, "tp"),
            P("ep", None),
            P(),
            P("ep", None),
            P("ep"),
            P("ep", None),
            P("ep", None, "tp"),
            P("ep", None, "tp"),
            P("ep", None, "tp"),
        ),
        out_specs=(P("ep", "tp"), P("ep", "tp")),
        check_vma=False,
    )
```

```python
import functools

import jax
import jax.numpy as jnp
from jax import lax
from jax.experimental import pallas as pl
from jax.experimental.pallas import tpu as pltpu
from jax.sharding import PartitionSpec as P

EXPERTS = 32
TOP = 2
MOE_DEV = 128
CAP = 16

MESH = pl.DeviceIdType.MESH

LANES = 128
CONV_CHUNKS = 6
EARLY_CHUNKS = 4
PROMPT_CHUNKS = 3

epsilon = 1e-06


def slot_numbers(route_experts):
    picked = route_experts.reshape(-1, MOE_DEV * TOP)
    onehot = (picked[:, :, None] == jnp.arange(EXPERTS, dtype=jnp.int32)).astype(jnp.bfloat16)
    order = jnp.arange(MOE_DEV * TOP, dtype=jnp.int32)
    earlier = (order[:, None] > order[None, :]).astype(jnp.bfloat16)
    before = jnp.einsum("ij,bje->bie", earlier, onehot, preferred_element_type=jnp.float32)
    positions = jnp.sum(before * onehot.astype(jnp.float32), axis=2).astype(jnp.int32)
    return (picked * CAP + positions).reshape(-1, MOE_DEV, TOP)


def on_line(place, order, length):
    upper = 2 * place // length
    short = place + upper * (length - 1 - 2 * place)
    beyond = (order - 2 * short - 1 + length) // length
    both = place + (1 - 2 * upper) * (2 * (order % 2) - 1) * ((order + 1) // 2)
    single = place + (1 - 2 * upper) * (order - short)
    return both + beyond * (single - both)


def fused_kernel(
    count,
    reach,
    tokens_hbm,
    expert_gain,
    routes,
    gate_hbm,
    up_hbm,
    down_hbm,
    value_hbm,
    switch_hbm,
    taps,
    conv_gain,
    conv_bias,
    projection_hbm,
    returned,
    gathered,
    projected,
    blocks,
    block_routes,
    spare,
    normed,
    crossing,
    landed,
    gate,
    up,
    down,
    hidden,
    result,
    value,
    switch,
    halo,
    gated,
    mixed,
    active,
    load_sem,
    conv_load,
    halo_send,
    halo_recv,
    route_send,
    route_recv,
    hop_send,
    hop_recv,
    cross_send,
    cross_recv,
    side_send,
    side_recv,
    near_send,
    near_recv,
    unit_send,
    unit_recv,
    back_send,
    back_recv,
    conv_kept,
    conv_send,
    conv_recv,
    project_load,
    project_kept,
):
    group, quarter = lax.axis_index("ep"), lax.axis_index("tp")
    quarters = landed.shape[1]
    near, side = quarter + 1 - 2 * (quarter % 2), (quarter + 2) % 4
    length = count // 2
    place, across = group // 2, group % 2
    other = place * 2 + 1 - across
    local = gate.shape[0]
    size = landed.shape[2]
    width = landed.shape[3]
    rows_per = value.shape[1]
    border = halo.shape[1]
    total = count * quarters
    flat = group * quarters + quarter
    after, before = (flat + 1) % total, (flat + total - 1) % total

    loads = [
        pltpu.make_async_copy(source, target, load_sem.at[number])
        for number, (source, target) in enumerate(
            [
                (tokens_hbm.at[pl.ds(quarter * MOE_DEV, MOE_DEV)], blocks.at[place]),
                (gate_hbm, gate),
                (up_hbm, up),
                (down_hbm, down),
            ]
        )
    ]
    loads[0].start()

    barrier = pltpu.get_barrier_semaphore()

    def greet(m, carry):
        pl.semaphore_signal(
            barrier, inc=1, device_id=((group + m) % count, quarter), device_id_type=MESH
        )
        return carry

    lax.fori_loop(1, count, greet, 0)
    for member in (near, side):
        pl.semaphore_signal(barrier, inc=1, device_id=(group, member), device_id_type=MESH)
    for member in (after, before):
        pl.semaphore_signal(
            barrier,
            inc=1,
            device_id=(member // quarters, member % quarters),
            device_id_type=MESH,
        )

    def conv_loads(c):
        rows = pl.ds(c * rows_per, rows_per)
        return [
            pltpu.make_async_copy(source.at[rows], target.at[c % 2], conv_load.at[number, c % 2])
            for number, (source, target) in enumerate([(value_hbm, value), (switch_hbm, switch)])
        ]

    for load in conv_loads(0):
        load.start()
    pl.semaphore_wait(barrier, count + 3)

    def copy(source, target, send, recv, device):
        return pltpu.make_async_remote_copy(
            src_ref=source,
            dst_ref=target,
            send_sem=send,
            recv_sem=recv,
            device_id=device,
            device_id_type=MESH,
        )

    def hop(origin, way):
        device = ((place + 1 - 2 * way) * 2 + across, quarter)
        spot = blocks.at[origin]
        return copy(spot, spot, hop_send.at[origin, way], hop_recv.at[origin], device)

    def route(m):
        device = ((place + m) % length * 2 + across, quarter)
        spot = block_routes.at[place]
        return copy(routes.at[quarter], spot, route_send.at[m], route_recv.at[place], device)

    def route_from(origin):
        spot = block_routes.at[origin]
        return copy(
            routes.at[quarter], spot, route_send.at[0], route_recv.at[origin], (other, quarter)
        )

    def edge(number):
        source = (value_hbm, switch_hbm)[number]
        last = source.at[pl.ds(source.shape[0] - border, border)]
        device = (after // quarters, after % quarters)
        return copy(last, halo.at[number], halo_send.at[number], halo_recv.at[number], device)

    def cross(order):
        spot = landed.at[2 * order + 1, quarter]
        send, recv = cross_send.at[order], cross_recv.at[order]
        return copy(crossing.at[order], spot, send, recv, (other, quarter))

    def cross_side():
        spot = landed.at[1, side]
        send, recv = cross_send.at[length], cross_recv.at[length]
        return copy(crossing.at[length], spot, send, recv, (other, quarter))

    def to_side(m):
        spot = landed.at[m, quarter]
        return copy(spot, spot, side_send.at[m], side_recv.at[m], (group, side))

    def to_near(m, number):
        spot = landed.at[m, (quarter, side)[number]]
        send, recv = near_send.at[m, number], near_recv.at[m, number]
        return copy(spot, spot, send, recv, (group, near))

    def units(p, number):
        spot = hidden.at[p, (quarter, quarter, side)[number]]
        send, recv = unit_send.at[p, number], unit_recv.at[p, number]
        return copy(spot, spot, send, recv, (group, (side, near, near)[number]))

    def back(m):
        home = on_line(place, m // 2, length) * 2 + (across + m) % 2
        spot = returned.at[group]
        return copy(result.at[m], spot, back_send.at[m], back_recv.at[group], (home, quarter))

    def back_from(origin):
        spot = returned.at[origin]
        return copy(result.at[0], spot, back_send.at[0], back_recv.at[origin], (origin, quarter))

    def kept():
        return pltpu.make_async_copy(result.at[0], returned.at[group], load_sem.at[5])

    def conv_share(c, number):
        rows = pl.ds(c * rows_per, rows_per)
        spot = gathered.at[(quarter, quarter, side)[number], rows]
        source = (active.at[c], active.at[c], spot)[number]
        send, recv = conv_send.at[c, number], conv_recv.at[c, number]
        return copy(source, spot, send, recv, (group, (side, near, near)[number]))

    def conv_keep(c):
        spot = gathered.at[quarter, pl.ds(c * rows_per, rows_per)]
        return pltpu.make_async_copy(active.at[c], spot, conv_kept.at[c])

    def start_route(m, carry):
        route(m).start()
        return carry

    lax.fori_loop(1, length, start_route, 0)
    edge(0).start()
    edge(1).start()
    loads[0].wait()

    @pl.when(place < length - 1)
    def _():
        hop(place, 0).start()

    @pl.when(place > 0)
    def _():
        hop(place, 1).start()

    for load in loads[1:]:
        load.start()

    def arrive(distance):
        lower, upper = place - distance, place + distance

        @pl.when(lower >= 0)
        def _():
            hop(lower, 0).wait_recv()

            @pl.when(place < length - 1)
            def _():
                hop(lower, 0).start()

        @pl.when(upper < length)
        def _():
            hop(upper, 1).wait_recv()

            @pl.when(place > 0)
            def _():
                hop(upper, 1).start()

    def normalize(source):
        def some_rows(q, carry):
            rows = pl.ds(pl.multiple_of(q * 16, 16), 16)
            widened = source[rows, :].astype(jnp.float32)
            inverse_rms = lax.rsqrt(jnp.mean(widened * widened, axis=-1, keepdims=True) + epsilon)
            normed[rows, :] = (widened * inverse_rms * expert_gain[...]).astype(jnp.bfloat16)
            return carry

        lax.fori_loop(0, MOE_DEV // 16, some_rows, 0)

    def chosen(table):
        slot = lax.broadcasted_iota(jnp.int32, (2 * size, MOE_DEV), 0)
        second = (slot >= size).astype(jnp.int32)
        within = slot - second * size
        number = (group + second * (other - group)) * local + lax.shift_right_logical(
            within, CAP.bit_length() - 1
        )
        named = (table[0:1, :] == number) | (table[1:2, :] == number)
        row = lax.broadcasted_iota(jnp.int32, (MOE_DEV, MOE_DEV), 0)
        column = lax.broadcasted_iota(jnp.int32, (MOE_DEV, MOE_DEV), 1)
        earlier = jnp.where(row < column, 1.0, 0.0).astype(jnp.bfloat16)
        ones = jnp.where(named, 1.0, 0.0)
        taken = jnp.dot(ones.astype(jnp.bfloat16), earlier, preferred_element_type=jnp.float32)
        wanted = (within & (CAP - 1)).astype(jnp.float32)
        return jnp.where(taken == wanted, ones, 0.0).astype(jnp.bfloat16)

    def fill(table, spot, order, own_only):
        picks = chosen(table)
        piece = 1024

        def some_columns(q, carry):
            columns = pl.ds(pl.multiple_of(q * piece, piece), piece)
            part = jnp.dot(picks, normed[:, columns], preferred_element_type=jnp.float32)
            part = part.astype(jnp.bfloat16)
            landed[spot[0], spot[1], :, columns] = part[:size]

            @pl.when(own_only == 0)
            def _():
                crossing[order, :, columns] = part[size:]

            return carry

        lax.fori_loop(0, width // piece, some_columns, 0)

    def own_block(k, carry):
        member = (quarter + 2 * (k % 2) + k // 2) % quarters

        @pl.when(k == 0)
        def _():
            normalize(blocks.at[place])

        @pl.when(k > 0)
        def _():
            rows = pl.ds(member * MOE_DEV, MOE_DEV)
            load = pltpu.make_async_copy(tokens_hbm.at[rows], spare, load_sem.at[4])
            load.start()
            load.wait()
            normalize(spare)

        both = k // 2
        fill(routes.at[member], (0, member), (1 - both) * k * length, both)

        @pl.when(k == 0)
        def _():
            cross(0).start()

        @pl.when(k == 1)
        def _():
            cross_side().start()

        return carry

    lax.fori_loop(0, 2, own_block, 0)

    def conv_chunk(c):
        pieces = gated.shape[0]
        slot = c % 2

        @pl.when(c == 0)
        def _():
            edge(0).wait_recv()
            edge(1).wait_recv()

            def first_rows(q, carry):
                lanes = pl.ds(pl.multiple_of(q * LANES, LANES), LANES)
                left = halo[0, :, lanes].astype(jnp.float32)
                right = jax.nn.sigmoid(halo[1, :, lanes].astype(jnp.float32))
                product = (left * right).astype(jnp.bfloat16).astype(jnp.float32)
                gated[q, 0:border, :] = jnp.where(flat == 0, 0.0, product)
                return carry

            lax.fori_loop(0, pieces, first_rows, 0)

        @pl.when(c > 0)
        def _():
            def last_rows(q, carry):
                gated[q, 0:border, :] = gated[q, rows_per : rows_per + border, :]
                return carry

            lax.fori_loop(0, pieces, last_rows, 0)

        for load in conv_loads(c):
            load.wait()

        @pl.when(c + 1 < CONV_CHUNKS)
        def _():
            for load in conv_loads(c + 1):
                load.start()

        def mix(q, sums):
            lanes = pl.ds(pl.multiple_of(q * LANES, LANES), LANES)
            left = value[slot, :, lanes].astype(jnp.float32)
            right = jax.nn.sigmoid(switch[slot, :, lanes].astype(jnp.float32))
            gated[q, border : border + rows_per, :] = (
                (left * right).astype(jnp.bfloat16).astype(jnp.float32)
            )
            amount = jnp.zeros((rows_per, LANES), jnp.float32)
            for tap in range(reach + 1):
                window = gated[q, border - tap : border - tap + rows_per, :]
                amount = amount + taps[tap : tap + 1, lanes] * window
            mixed[q] = amount
            return sums + amount

        sums = lax.fori_loop(0, pieces, mix, jnp.zeros((rows_per, LANES), jnp.float32))
        channels = pieces * LANES
        mean = jnp.sum(sums, axis=-1, keepdims=True) / channels

        def spread_of(q, squares):
            center = mixed[q] - mean
            return squares + center * center

        squares = lax.fori_loop(0, pieces, spread_of, jnp.zeros((rows_per, LANES), jnp.float32))
        spread = jnp.sum(squares, axis=-1, keepdims=True) / channels
        scale = lax.rsqrt(spread + epsilon)

        def activate(q, carry):
            lanes = pl.ds(pl.multiple_of(q * LANES, LANES), LANES)
            level = (mixed[q] - mean) * scale * conv_gain[:, lanes] + conv_bias[:, lanes]
            active[c, :, lanes] = (level * jax.nn.sigmoid(level)).astype(jnp.bfloat16)
            return carry

        lax.fori_loop(0, pieces, activate, 0)

        @pl.when(c < PROMPT_CHUNKS)
        def _():
            conv_share(c, 0).start()

        conv_share(c, 1).start()
        conv_keep(c).start()

    def early(c, carry):
        conv_chunk(c)
        return carry

    lax.fori_loop(0, EARLY_CHUNKS, early, 0)
    lax.fori_loop(2, quarters, own_block, 0)

    def to_hidden(p):
        for e in range(local):
            rows = landed[p, :, e * CAP : (e + 1) * CAP, :]
            rows = rows.reshape(rows.shape[0] * CAP, rows.shape[2])
            gate_part = jnp.dot(rows, gate[e], preferred_element_type=jnp.float32)
            up_part = jnp.dot(rows, up[e], preferred_element_type=jnp.float32)
            part = (gate_part / (1.0 + jnp.exp(-gate_part)) * up_part).astype(jnp.bfloat16)
            part = part.reshape(-1, CAP, part.shape[1])
            hidden[p, quarter, :, e * CAP : (e + 1) * CAP, :] = part

    def to_result(p):
        for e in range(local):
            parts = [hidden[p, t, :, e * CAP : (e + 1) * CAP, :] for t in range(hidden.shape[1])]
            parts = [part.reshape(-1, part.shape[2]) for part in parts]
            total = jnp.dot(
                jnp.concatenate(parts, axis=1), down[e], preferred_element_type=jnp.float32
            )
            total = total.astype(jnp.bfloat16).reshape(-1, CAP, total.shape[1])
            result[p, :, e * CAP : (e + 1) * CAP, :] = total

    loads[1].wait()
    loads[2].wait()
    loads[3].wait()

    def step(j, carry):
        @pl.when((j >= 2) & (j < count) & (j % 2 == 0))
        def _():
            order = j // 2
            origin = on_line(place, order, length)
            arrive(order)
            normalize(blocks.at[origin])
            route_from(origin).wait_recv()
            fill(block_routes.at[origin], (j, quarter), order, 0)
            cross(order).start()

        @pl.when((j >= 1) & (j < count) & (j % 2 == 1))
        def _():
            cross(j // 2).wait_recv()

        @pl.when((j >= 2) & (j < count))
        def _():
            to_side(j).start()

        @pl.when((j >= 1) & (j < count))
        def _():
            to_near(j, 0).start()

        @pl.when((j >= 2) & (j < count + 1))
        def _():
            @pl.when(j == 2)
            def _():
                cross_side().wait_recv()

            @pl.when(j > 2)
            def _():
                to_side(j - 1).wait_recv()

            to_near(j - 1, 1).start()

        @pl.when((j >= 3) & (j < count + 3))
        def _():
            units(j - 3, 0).wait_recv()
            units(j - 3, 2).start()

        @pl.when((j >= 3) & (j < count + 2))
        def _():
            to_near(j - 2, 0).wait_recv()
            to_near(j - 2, 1).wait_recv()

        @pl.when((j >= 2) & (j < count + 2))
        def _():
            to_hidden(j - 2)

        @pl.when((j >= 3) & (j < count + 3))
        def _():
            units(j - 3, 1).wait_recv()
            units(j - 3, 2).wait_recv()
            to_result(j - 3)

        @pl.when((j >= 2) & (j < count + 2))
        def _():
            units(j - 2, 0).start()
            units(j - 2, 1).start()

        @pl.when((j >= 2) & (j < 2 + CONV_CHUNKS - EARLY_CHUNKS))
        def _():
            conv_chunk(j - 2 + EARLY_CHUNKS)

        @pl.when(j == 3)
        def _():
            kept().start()

        @pl.when((j >= 4) & (j < count + 3))
        def _():
            back(j - 3).start()

        @pl.when((j >= count) & (j < count + 1))
        def _():
            for c in range(PROMPT_CHUNKS):
                conv_share(c, 0).wait_recv()
                conv_share(c, 2).start()

        @pl.when((j >= count + 1) & (j < count + 2))
        def _():
            for c in range(PROMPT_CHUNKS, CONV_CHUNKS):
                conv_share(c, 0).start()

        return carry

    lax.fori_loop(1, count + 3, step, 0)

    def finish_sides(m, carry):
        @pl.when(m > 1)
        def _():
            to_side(m).wait_send()

        to_near(m, 0).wait_send()
        to_near(m, 1).wait_send()
        return carry

    lax.fori_loop(1, count, finish_sides, 0)
    channels, features = active.shape[2], down.shape[2]
    columns = gate.shape[2]

    def project_loads():
        return [
            pltpu.make_async_copy(
                projection_hbm.at[:, pl.ds(q * columns, columns)],
                gate.at[q, pl.ds(0, channels)],
                project_load.at[quarters + q],
            )
            for q in range(features // columns)
        ]

    def kept_out(c, q):
        rows = pl.ds(q * active.shape[0] * rows_per + c * rows_per, rows_per)
        source = landed.at[c, q, :, pl.ds(channels, features)]
        return pltpu.make_async_copy(source, projected.at[rows], project_kept.at[c, q])

    if projected is not None:
        for load in project_loads():
            load.start()

    def settle(c, carry):
        @pl.when(c >= PROMPT_CHUNKS)
        def _():
            conv_share(c, 0).wait_recv()
            conv_share(c, 2).start()

        conv_keep(c).wait()
        conv_share(c, 1).wait_recv()
        conv_share(c, 2).wait_recv()
        if projected is not None:
            rows = pl.ds(c * rows_per, rows_per)
            fetches = [
                pltpu.make_async_copy(
                    gathered.at[q, rows],
                    landed.at[c, q, :, pl.ds(0, channels)],
                    project_load.at[q],
                )
                for q in range(quarters)
            ]
            for fetch in fetches:
                fetch.start()

            @pl.when(c == 0)
            def _():
                for load in project_loads():
                    load.wait()

            for fetch in fetches:
                fetch.wait()
            whole = landed[c, :, :, 0:channels].reshape(quarters * size, channels)
            for q in range(features // columns):
                part = jnp.dot(
                    whole, gate[q, 0:channels, :], preferred_element_type=jnp.float32
                )
                part = part.astype(jnp.bfloat16).reshape(quarters, size, columns)
                start = channels + q * columns
                landed[c, :, :, start : start + columns] = part
            for q in range(quarters):
                kept_out(c, q).start()
        return carry

    lax.fori_loop(0, CONV_CHUNKS, settle, 0)

    @pl.when(place < length - 1)
    def _():
        hop(place, 0).wait_send()

    @pl.when(place > 0)
    def _():
        hop(place, 1).wait_send()

    def finish_line(m, carry):
        route(m).wait_send()
        origin = on_line(place, m, length)

        @pl.when((origin < place) & (place < length - 1))
        def _():
            hop(origin, 0).wait_send()

        @pl.when((origin > place) & (place > 0))
        def _():
            hop(origin, 1).wait_send()

        cross(m).wait_send()
        return carry

    cross(0).wait_send()
    cross_side().wait_send()
    lax.fori_loop(1, length, finish_line, 0)
    edge(0).wait_send()
    edge(1).wait_send()

    def finish_conv(c, carry):
        for number in range(3):
            conv_share(c, number).wait_send()
        if projected is not None:
            for q in range(quarters):
                kept_out(c, q).wait()
        return carry

    lax.fori_loop(0, CONV_CHUNKS, finish_conv, 0)

    def finish_units(p, carry):
        for number in range(3):
            units(p, number).wait_send()
        return carry

    lax.fori_loop(0, count, finish_units, 0)

    def finish(m, carry):
        back(m).wait_send()
        back_from((group + m) % count).wait_recv()
        return carry

    lax.fori_loop(1, count, finish, 0)
    kept().wait()


def fused(
    tokens,
    expert_gain,
    routes,
    gate_weight,
    up_weight,
    down_weight,
    conv_value,
    conv_gate,
    conv_taps,
    conv_gain,
    conv_bias,
    projection,
    count,
):
    width = tokens.shape[1]
    quarters = tokens.shape[0] // MOE_DEV
    local, units, features = gate_weight.shape[0], gate_weight.shape[2], down_weight.shape[2]
    size = local * CAP
    length = count // 2
    positions, channels = conv_value.shape
    rows_per = positions // CONV_CHUNKS
    reach = conv_taps.shape[0] - 1
    border = -(-reach // 16) * 16
    rows = count * quarters * size
    dma = pltpu.SemaphoreType.DMA
    anywhere = pl.BlockSpec(memory_space=pl.ANY)
    inside = pl.BlockSpec(memory_space=pltpu.VMEM)
    inside_too = (
        rows_per == size
        and CONV_CHUNKS <= count
        and channels + features <= width
        and features == local * units
    )

    def kernel(*refs):
        if inside_too:
            return fused_kernel(count, reach, *refs)
        return fused_kernel(count, reach, *refs[:14], None, *refs[14:])

    out_shape = (
        jax.ShapeDtypeStruct((count, quarters, size, features), jnp.bfloat16),
        jax.ShapeDtypeStruct((quarters, positions, channels), jnp.bfloat16),
        jax.ShapeDtypeStruct((quarters * positions, features), jnp.bfloat16),
    )
    outputs = 2 + inside_too
    results = pl.pallas_call(
        kernel,
        out_shape=out_shape[:outputs],
        in_specs=[
            anywhere,
            inside,
            inside,
            anywhere,
            anywhere,
            anywhere,
            anywhere,
            anywhere,
            inside,
            inside,
            inside,
            anywhere,
        ],
        out_specs=(anywhere,) * outputs,
        scratch_shapes=[
            pltpu.VMEM((length, MOE_DEV, width), jnp.bfloat16),
            pltpu.VMEM((length,) + routes.shape[1:], jnp.int32),
            pltpu.VMEM((MOE_DEV, width), jnp.bfloat16),
            pltpu.VMEM((MOE_DEV, width), jnp.bfloat16),
            pltpu.VMEM((length + 1, size, width), jnp.bfloat16),
            pltpu.VMEM((count, quarters, size, width), jnp.bfloat16),
            pltpu.VMEM(gate_weight.shape, jnp.bfloat16),
            pltpu.VMEM(up_weight.shape, jnp.bfloat16),
            pltpu.VMEM(down_weight.shape, jnp.bfloat16),
            pltpu.VMEM((count, quarters, quarters, size, units), jnp.bfloat16),
            pltpu.VMEM((count, quarters, size, features), jnp.bfloat16),
            pltpu.VMEM((2, rows_per, channels), jnp.bfloat16),
            pltpu.VMEM((2, rows_per, channels), jnp.bfloat16),
            pltpu.VMEM((2, border, channels), jnp.bfloat16),
            pltpu.VMEM((channels // LANES, border + rows_per, LANES), jnp.float32),
            pltpu.VMEM((channels // LANES, rows_per, LANES), jnp.float32),
            pltpu.VMEM((CONV_CHUNKS, rows_per, channels), jnp.bfloat16),
            dma((6,)),
            dma((2, 2)),
            dma((2,)),
            dma((2,)),
            dma((length,)),
            dma((length,)),
            dma((length, 2)),
            dma((length,)),
            dma((length + 1,)),
            dma((length + 1,)),
            dma((count,)),
            dma((count,)),
            dma((count, 2)),
            dma((count, 2)),
            dma((count, 3)),
            dma((count, 3)),
            dma((count,)),
            dma((count,)),
            dma((CONV_CHUNKS,)),
            dma((CONV_CHUNKS, 3)),
            dma((CONV_CHUNKS, 3)),
            dma((quarters + max(1, features // units),)),
            dma((CONV_CHUNKS, quarters)),
        ],
        compiler_params=pltpu.CompilerParams(
            collective_id=0, has_side_effects=True, vmem_limit_bytes=67_043_328
        ),
        cost_estimate=pl.CostEstimate(
            flops=40 * rows * width * units, bytes_accessed=250_000_000, transcendentals=0
        ),
    )(
        tokens,
        expert_gain,
        routes,
        gate_weight,
        up_weight,
        down_weight,
        conv_value,
        conv_gate,
        conv_taps,
        conv_gain,
        conv_bias,
        projection,
    )
    if inside_too:
        return results[0], results[2]
    projected = jnp.dot(
        results[1].reshape(-1, channels), projection, preferred_element_type=jnp.float32
    )
    return results[0], projected.astype(jnp.bfloat16)


def weighed(results, slots, share):
    wanted = jnp.arange(results.shape[0] * results.shape[2], dtype=jnp.int32)
    same = slots[:, :, :, None] == wanted[None, None, None, :]
    weights = jnp.sum(jnp.where(same, share[:, :, :, None], 0.0), axis=2)
    high = weights.astype(jnp.bfloat16)
    low = (weights - high.astype(jnp.float32)).astype(jnp.bfloat16)
    both = jnp.concatenate([high, low], axis=1)
    both = both.reshape(both.shape[:2] + (results.shape[0], results.shape[2]))
    total = jnp.einsum("qrks,kqsd->qrd", both, results, preferred_element_type=jnp.float32)
    return total[:, : total.shape[1] // 2] + total[:, total.shape[1] // 2 :]


def on_device(
    conv_value,
    conv_gate,
    conv_taps,
    conv_gain,
    conv_bias,
    conv_projection,
    expert_input,
    expert_gain,
    route_experts,
    group_gate,
    expert_gate,
    gate_weight,
    up_weight,
    down_weight,
):
    count = lax.axis_size("ep")
    slots = slot_numbers(route_experts)
    quarters = slots.shape[0]
    share = group_gate[:, None] * expert_gate / jnp.sum(expert_gate, axis=1, keepdims=True)
    share = share.reshape(slots.shape)
    routes = jnp.swapaxes(route_experts.reshape(quarters, MOE_DEV, TOP), 1, 2)
    results, conv_out = fused(
        expert_input,
        expert_gain[None],
        routes,
        gate_weight,
        up_weight,
        down_weight,
        conv_value,
        conv_gate,
        conv_taps,
        conv_gain[None],
        conv_bias[None],
        conv_projection,
        count,
    )
    total = weighed(results, slots, share)
    expert_out = total.reshape(quarters * MOE_DEV, -1).astype(jnp.bfloat16)
    return (conv_out, expert_out)


def solution(mesh):
    return jax.shard_map(
        on_device,
        mesh=mesh,
        in_specs=(
            P(("ep", "tp"), None),
            P(("ep", "tp"), None),
            P(),
            P(),
            P(),
            P(None, "tp"),
            P("ep", None),
            P(),
            P("ep", None),
            P("ep"),
            P("ep", None),
            P("ep", None, "tp"),
            P("ep", None, "tp"),
            P("ep", None, "tp"),
        ),
        out_specs=(P("ep", "tp"), P("ep", "tp")),
        check_vma=False,
    )
```

```python
import functools

import jax
import jax.numpy as jnp
from jax import lax
from jax.experimental import pallas as pl
from jax.experimental.pallas import tpu as pltpu
from jax.sharding import PartitionSpec as P

TOP = 2
MOE_DEV = 128
CAP = 16

MESH = pl.DeviceIdType.MESH

LANES = 128
CONV_CHUNKS = 6
EARLY_CHUNKS = 2
PROMPT_CHUNKS = 2

epsilon = 1e-06


def on_line(place, order, length):
    upper = 2 * place // length
    short = place + upper * (length - 1 - 2 * place)
    beyond = (order - 2 * short - 1 + length) // length
    both = place + (1 - 2 * upper) * (2 * (order % 2) - 1) * ((order + 1) // 2)
    single = place + (1 - 2 * upper) * (order - short)
    return both + beyond * (single - both)


def fused_kernel(
    count,
    reach,
    tokens_hbm,
    expert_gain,
    routes,
    gate_hbm,
    up_hbm,
    down_hbm,
    value_hbm,
    switch_hbm,
    taps,
    conv_gain,
    conv_bias,
    projection_hbm,
    group_gate,
    expert_gate,
    returned,
    gathered,
    combined,
    projected,
    blocks,
    block_routes,
    spare,
    normed,
    crossing,
    landed,
    gate,
    up,
    down,
    hidden,
    result,
    value,
    switch,
    halo,
    gated,
    mixed,
    active,
    load_sem,
    conv_load,
    halo_send,
    halo_recv,
    route_send,
    route_recv,
    hop_send,
    hop_recv,
    cross_send,
    cross_recv,
    side_send,
    side_recv,
    near_send,
    near_recv,
    unit_send,
    unit_recv,
    back_send,
    back_recv,
    conv_kept,
    conv_send,
    conv_recv,
    project_load,
    project_kept,
    fetch_sem,
    combine_kept,
):
    group, quarter = lax.axis_index("ep"), lax.axis_index("tp")
    quarters = landed.shape[1]
    near, side = quarter + 1 - 2 * (quarter % 2), (quarter + 2) % 4
    length = count // 2
    place, across = group // 2, group % 2
    other = place * 2 + 1 - across
    local = gate.shape[0]
    size = landed.shape[2]
    width = landed.shape[3]
    rows_per = value.shape[1]
    border = halo.shape[1]
    total = count * quarters
    flat = group * quarters + quarter
    after, before = (flat + 1) % total, (flat + total - 1) % total

    loads = [
        pltpu.make_async_copy(source, target, load_sem.at[number])
        for number, (source, target) in enumerate(
            [
                (tokens_hbm.at[pl.ds(quarter * MOE_DEV, MOE_DEV)], blocks.at[place]),
                (gate_hbm, gate),
                (up_hbm, up),
                (down_hbm, down),
            ]
        )
    ]
    loads[0].start()

    barrier = pltpu.get_barrier_semaphore()

    def greet(m, carry):
        pl.semaphore_signal(
            barrier, inc=1, device_id=((group + m) % count, quarter), device_id_type=MESH
        )
        return carry

    lax.fori_loop(1, count, greet, 0)
    for member in (near, side):
        pl.semaphore_signal(barrier, inc=1, device_id=(group, member), device_id_type=MESH)
    for member in (after, before):
        pl.semaphore_signal(
            barrier,
            inc=1,
            device_id=(member // quarters, member % quarters),
            device_id_type=MESH,
        )

    def conv_loads(c):
        rows = pl.ds(c * rows_per, rows_per)
        return [
            pltpu.make_async_copy(source.at[rows], target.at[c % 2], conv_load.at[number, c % 2])
            for number, (source, target) in enumerate([(value_hbm, value), (switch_hbm, switch)])
        ]

    for load in conv_loads(0):
        load.start()
    pl.semaphore_wait(barrier, count + 3)

    def copy(source, target, send, recv, device):
        return pltpu.make_async_remote_copy(
            src_ref=source,
            dst_ref=target,
            send_sem=send,
            recv_sem=recv,
            device_id=device,
            device_id_type=MESH,
        )

    def hop(origin, way):
        device = ((place + 1 - 2 * way) * 2 + across, quarter)
        spot = blocks.at[origin]
        return copy(spot, spot, hop_send.at[origin, way], hop_recv.at[origin], device)

    def route(m):
        device = ((place + m) % length * 2 + across, quarter)
        spot = block_routes.at[place]
        return copy(routes.at[quarter], spot, route_send.at[m], route_recv.at[place], device)

    def route_from(origin):
        spot = block_routes.at[origin]
        return copy(
            routes.at[quarter], spot, route_send.at[0], route_recv.at[origin], (other, quarter)
        )

    def edge(number):
        source = (value_hbm, switch_hbm)[number]
        last = source.at[pl.ds(source.shape[0] - border, border)]
        device = (after // quarters, after % quarters)
        return copy(last, halo.at[number], halo_send.at[number], halo_recv.at[number], device)

    def cross(order):
        spot = landed.at[2 * order + 1, quarter]
        send, recv = cross_send.at[order], cross_recv.at[order]
        return copy(crossing.at[order], spot, send, recv, (other, quarter))

    def cross_side():
        spot = landed.at[1, side]
        send, recv = cross_send.at[length], cross_recv.at[length]
        return copy(crossing.at[length], spot, send, recv, (other, quarter))

    def to_side(m):
        spot = landed.at[m, quarter]
        return copy(spot, spot, side_send.at[m], side_recv.at[m], (group, side))

    def to_near(m, number):
        spot = landed.at[m, (quarter, side)[number]]
        send, recv = near_send.at[m, number], near_recv.at[m, number]
        return copy(spot, spot, send, recv, (group, near))

    def units(p, number):
        spot = hidden.at[p, (quarter, quarter, side)[number]]
        send, recv = unit_send.at[p, number], unit_recv.at[p, number]
        return copy(spot, spot, send, recv, (group, (side, near, near)[number]))

    def back(m):
        home = on_line(place, m // 2, length) * 2 + (across + m) % 2
        spot = returned.at[group]
        return copy(result.at[m], spot, back_send.at[m], back_recv.at[group], (home, quarter))

    def back_from(origin):
        spot = returned.at[origin]
        return copy(result.at[0], spot, back_send.at[0], back_recv.at[origin], (origin, quarter))

    def kept():
        return pltpu.make_async_copy(result.at[0], returned.at[group], load_sem.at[5])

    def conv_share(c, number):
        rows = pl.ds(c * rows_per, rows_per)
        spot = gathered.at[(quarter, quarter, side)[number], rows]
        source = (active.at[c], active.at[c], spot)[number]
        send, recv = conv_send.at[c, number], conv_recv.at[c, number]
        return copy(source, spot, send, recv, (group, (side, near, near)[number]))

    def conv_keep(c):
        spot = gathered.at[quarter, pl.ds(c * rows_per, rows_per)]
        return pltpu.make_async_copy(active.at[c], spot, conv_kept.at[c])

    def start_route(m, carry):
        route(m).start()
        return carry

    lax.fori_loop(1, length, start_route, 0)
    edge(0).start()
    edge(1).start()
    loads[0].wait()

    @pl.when(place < length - 1)
    def _():
        hop(place, 0).start()

    @pl.when(place > 0)
    def _():
        hop(place, 1).start()

    for load in loads[1:]:
        load.start()

    def arrive(distance):
        lower, upper = place - distance, place + distance

        @pl.when(lower >= 0)
        def _():
            hop(lower, 0).wait_recv()

            @pl.when(place < length - 1)
            def _():
                hop(lower, 0).start()

        @pl.when(upper < length)
        def _():
            hop(upper, 1).wait_recv()

            @pl.when(place > 0)
            def _():
                hop(upper, 1).start()

    def normalize(source):
        def some_rows(q, carry):
            rows = pl.ds(pl.multiple_of(q * 16, 16), 16)
            widened = source[rows, :].astype(jnp.float32)
            inverse_rms = lax.rsqrt(jnp.mean(widened * widened, axis=-1, keepdims=True) + epsilon)
            normed[rows, 0:width] = (widened * inverse_rms * expert_gain[...]).astype(jnp.bfloat16)
            return carry

        lax.fori_loop(0, MOE_DEV // 16, some_rows, 0)

    def earlier_rows():
        row = lax.broadcasted_iota(jnp.int32, (MOE_DEV, MOE_DEV), 0)
        column = lax.broadcasted_iota(jnp.int32, (MOE_DEV, MOE_DEV), 1)
        return jnp.where(row < column, 1.0, 0.0).astype(jnp.bfloat16)

    def chosen(table):
        slot = lax.broadcasted_iota(jnp.int32, (2 * size, MOE_DEV), 0)
        second = (slot >= size).astype(jnp.int32)
        within = slot - second * size
        number = (group + second * (other - group)) * local + lax.shift_right_logical(
            within, CAP.bit_length() - 1
        )
        named = (table[0:1, :] == number) | (table[1:2, :] == number)
        ones = jnp.where(named, 1.0, 0.0)
        taken = jnp.dot(
            ones.astype(jnp.bfloat16), earlier_rows(), preferred_element_type=jnp.float32
        )
        wanted = (within & (CAP - 1)).astype(jnp.float32)
        return jnp.where(taken == wanted, ones, 0.0).astype(jnp.bfloat16)

    def fill(table, spot, order, own_only):
        picks = chosen(table)
        piece = 1024

        def some_columns(q, carry):
            columns = pl.ds(pl.multiple_of(q * piece, piece), piece)
            part = jnp.dot(picks, normed[:, columns], preferred_element_type=jnp.float32)
            part = part.astype(jnp.bfloat16)
            landed[spot[0], spot[1], :, columns] = part[:size]

            @pl.when(own_only == 0)
            def _():
                crossing[order, :, columns] = part[size:]

            return carry

        lax.fori_loop(0, width // piece, some_columns, 0)

    def own_block(k, carry):
        member = (quarter + 2 * (k % 2) + k // 2) % quarters

        @pl.when(k == 0)
        def _():
            normalize(blocks.at[place])

        @pl.when(k > 0)
        def _():
            rows = pl.ds(member * MOE_DEV, MOE_DEV)
            load = pltpu.make_async_copy(
                tokens_hbm.at[rows], spare.at[:, pl.ds(0, width)], load_sem.at[4]
            )
            load.start()
            load.wait()
            normalize(spare.at[:, pl.ds(0, width)])

        both = k // 2
        fill(routes.at[member], (0, member), (1 - both) * k * length, both)

        @pl.when(k == 0)
        def _():
            cross(0).start()

        @pl.when(k == 1)
        def _():
            cross_side().start()

        return carry

    lax.fori_loop(0, 2, own_block, 0)

    def conv_chunk(c):
        pieces = gated.shape[0]
        slot = c % 2

        @pl.when(c == 0)
        def _():
            edge(0).wait_recv()
            edge(1).wait_recv()

            def first_rows(q, carry):
                lanes = pl.ds(pl.multiple_of(q * LANES, LANES), LANES)
                left = halo[0, :, lanes].astype(jnp.float32)
                right = jax.nn.sigmoid(halo[1, :, lanes].astype(jnp.float32))
                product = (left * right).astype(jnp.bfloat16).astype(jnp.float32)
                gated[q, 0:border, :] = jnp.where(flat == 0, 0.0, product)
                return carry

            lax.fori_loop(0, pieces, first_rows, 0)

        @pl.when(c > 0)
        def _():
            def last_rows(q, carry):
                gated[q, 0:border, :] = gated[q, rows_per : rows_per + border, :]
                return carry

            lax.fori_loop(0, pieces, last_rows, 0)

        for load in conv_loads(c):
            load.wait()

        @pl.when(c + 1 < CONV_CHUNKS)
        def _():
            for load in conv_loads(c + 1):
                load.start()

        def mix(q, sums):
            lanes = pl.ds(pl.multiple_of(q * LANES, LANES), LANES)
            left = value[slot, :, lanes].astype(jnp.float32)
            right = jax.nn.sigmoid(switch[slot, :, lanes].astype(jnp.float32))
            gated[q, border : border + rows_per, :] = (
                (left * right).astype(jnp.bfloat16).astype(jnp.float32)
            )
            amount = jnp.zeros((rows_per, LANES), jnp.float32)
            for tap in range(reach + 1):
                window = gated[q, border - tap : border - tap + rows_per, :]
                amount = amount + taps[tap : tap + 1, lanes] * window
            mixed[q] = amount
            return sums + amount

        sums = lax.fori_loop(0, pieces, mix, jnp.zeros((rows_per, LANES), jnp.float32))
        channels = pieces * LANES
        mean = jnp.sum(sums, axis=-1, keepdims=True) / channels

        def spread_of(q, squares):
            center = mixed[q] - mean
            return squares + center * center

        squares = lax.fori_loop(0, pieces, spread_of, jnp.zeros((rows_per, LANES), jnp.float32))
        spread = jnp.sum(squares, axis=-1, keepdims=True) / channels
        scale = lax.rsqrt(spread + epsilon)

        def activate(q, carry):
            lanes = pl.ds(pl.multiple_of(q * LANES, LANES), LANES)
            level = (mixed[q] - mean) * scale * conv_gain[:, lanes] + conv_bias[:, lanes]
            active[c, :, lanes] = (level * jax.nn.sigmoid(level)).astype(jnp.bfloat16)
            return carry

        lax.fori_loop(0, pieces, activate, 0)

        @pl.when(c < PROMPT_CHUNKS)
        def _():
            conv_share(c, 0).start()

        conv_share(c, 1).start()
        conv_keep(c).start()

    def early(c, carry):
        conv_chunk(c)
        return carry

    lax.fori_loop(0, EARLY_CHUNKS, early, 0)
    lax.fori_loop(2, quarters, own_block, 0)

    def to_hidden(p):
        for e in range(local):
            rows = landed[p, :, e * CAP : (e + 1) * CAP, :]
            rows = rows.reshape(rows.shape[0] * CAP, rows.shape[2])
            gate_part = jnp.dot(rows, gate[e], preferred_element_type=jnp.float32)
            up_part = jnp.dot(rows, up[e], preferred_element_type=jnp.float32)
            part = (gate_part / (1.0 + jnp.exp(-gate_part)) * up_part).astype(jnp.bfloat16)
            part = part.reshape(-1, CAP, part.shape[1])
            hidden[p, quarter, :, e * CAP : (e + 1) * CAP, :] = part

    def to_result(p):
        for e in range(local):
            parts = [hidden[p, t, :, e * CAP : (e + 1) * CAP, :] for t in range(hidden.shape[1])]
            parts = [part.reshape(-1, part.shape[2]) for part in parts]
            total = jnp.dot(
                jnp.concatenate(parts, axis=1), down[e], preferred_element_type=jnp.float32
            )
            total = total.astype(jnp.bfloat16).reshape(-1, CAP, total.shape[1])
            result[p, :, e * CAP : (e + 1) * CAP, :] = total

    loads[1].wait()
    loads[2].wait()
    loads[3].wait()

    nearest_end = place + 2 * place // length * (length - 1 - 2 * place)

    def step(j, carry):
        @pl.when((j >= 3) & (j < count + 2))
        def _():
            to_near(j - 2, 0).wait_recv()
            to_near(j - 2, 1).wait_recv()

        @pl.when((j >= 2) & (j < count + 2))
        def _():
            to_hidden(j - 2)
            units(j - 2, 0).start()
            units(j - 2, 1).start()

        @pl.when((j >= 2) & (j < count) & (j % 2 == 0))
        def _():
            order = j // 2
            origin = on_line(place, order, length)

            @pl.when((j == 2) | (nearest_end == 0))
            def _():
                arrive(order)

            normalize(blocks.at[origin])
            route_from(origin).wait_recv()
            fill(block_routes.at[origin], (j, quarter), order, 0)
            cross(order).start()

        @pl.when((j >= 1) & (j < count) & (j % 2 == 1))
        def _():
            cross(j // 2).wait_recv()

        @pl.when((j >= 2) & (j < count))
        def _():
            to_side(j).start()

        @pl.when((j >= 1) & (j < count))
        def _():
            to_near(j, 0).start()

        @pl.when((j >= 2) & (j < count + 1))
        def _():
            @pl.when(j == 2)
            def _():
                cross_side().wait_recv()

            @pl.when(j > 2)
            def _():
                to_side(j - 1).wait_recv()

            to_near(j - 1, 1).start()

        @pl.when((j >= 2) & (j < 2 + CONV_CHUNKS - EARLY_CHUNKS))
        def _():
            conv_chunk(j - 2 + EARLY_CHUNKS)

        @pl.when((j >= 2) & (j < count + 2))
        def _():
            units(j - 2, 0).wait_recv()
            units(j - 2, 2).start()
            units(j - 2, 1).wait_recv()
            units(j - 2, 2).wait_recv()
            to_result(j - 2)

        @pl.when(j == 2)
        def _():
            kept().start()

        @pl.when((j >= 3) & (j < count + 2))
        def _():
            back(j - 2).start()

        @pl.when((j >= 4) & (j < count) & (j % 2 == 0) & (nearest_end > 0))
        def _():
            arrive(j // 2)

        @pl.when((j >= count) & (j < count + 1))
        def _():
            for c in range(PROMPT_CHUNKS):
                conv_share(c, 0).wait_recv()
                conv_share(c, 2).start()

        @pl.when((j >= count + 1) & (j < count + 2))
        def _():
            for c in range(PROMPT_CHUNKS, CONV_CHUNKS):
                conv_share(c, 0).start()

        return carry

    lax.fori_loop(1, count + 2, step, 0)

    def finish_sides(m, carry):
        @pl.when(m > 1)
        def _():
            to_side(m).wait_send()

        to_near(m, 0).wait_send()
        to_near(m, 1).wait_send()
        return carry

    lax.fori_loop(1, count, finish_sides, 0)
    channels, features = active.shape[2], down.shape[2]
    columns = gate.shape[2]

    def project_loads():
        return [
            pltpu.make_async_copy(
                projection_hbm.at[:, pl.ds(q * columns, columns)],
                gate.at[q, pl.ds(0, channels)],
                project_load.at[CONV_CHUNKS, q],
            )
            for q in range(features // columns)
        ]

    def kept_out(c, q):
        rows = pl.ds(q * active.shape[0] * rows_per + c * rows_per, rows_per)
        source = landed.at[c, q, :, pl.ds(channels, features)]
        return pltpu.make_async_copy(source, projected.at[rows], project_kept.at[c, q])

    if projected is not None:
        for load in project_loads():
            load.start()

    def fetches(c):
        rows = pl.ds(c * rows_per, rows_per)
        return [
            pltpu.make_async_copy(
                gathered.at[q, rows],
                landed.at[c, q, :, pl.ds(0, channels)],
                project_load.at[c, q],
            )
            for q in range(quarters)
        ]

    def settle(c, carry):
        conv_keep(c).wait()
        conv_share(c, 1).wait_recv()
        conv_share(c, 2).wait_recv()
        if projected is not None:
            for load in fetches(c):
                load.start()
        return carry

    lax.fori_loop(0, PROMPT_CHUNKS, settle, 0)

    slots = count * size

    def picked(q, carry):
        slot = lax.broadcasted_iota(jnp.int32, (slots, MOE_DEV), 0)
        number = lax.shift_right_logical(slot, CAP.bit_length() - 1)
        table = routes.at[q]
        first, second = table[0:1, :] == number, table[1:2, :] == number
        ones = jnp.where(first | second, 1.0, 0.0).astype(jnp.bfloat16)
        taken = jnp.dot(ones, earlier_rows(), preferred_element_type=jnp.float32)
        wanted = (slot & (CAP - 1)).astype(jnp.float32)
        start = pl.multiple_of(q * 2 * slots, LANES)
        for k, named in enumerate((first, second)):
            picks = jnp.transpose(jnp.where(named & (taken == wanted), 1.0, 0.0))
            columns = pl.ds(pl.multiple_of(start + k * slots, LANES), slots)
            spare[:, columns] = picks.astype(jnp.bfloat16)
        return carry

    lax.fori_loop(0, quarters, picked, 0)

    if projected is not None:
        for load in project_loads():
            load.wait()

    def project(c, carry):
        if projected is not None:
            for load in fetches(c):
                load.wait()
            whole = landed[c, :, :, 0:channels].reshape(quarters * size, channels)
            for q in range(features // columns):
                part = jnp.dot(
                    whole, gate[q, 0:channels, :], preferred_element_type=jnp.float32
                )
                part = part.astype(jnp.bfloat16).reshape(quarters, size, columns)
                start = channels + q * columns
                landed[c, :, :, start : start + columns] = part
            for q in range(quarters):
                kept_out(c, q).start()

        @pl.when(c + PROMPT_CHUNKS < CONV_CHUNKS)
        def _():
            conv_share(c + PROMPT_CHUNKS, 0).wait_recv()
            conv_share(c + PROMPT_CHUNKS, 2).start()

        @pl.when((c >= 1) & (c + PROMPT_CHUNKS - 1 < CONV_CHUNKS))
        def _():
            settle(c + PROMPT_CHUNKS - 1, 0)

        return carry

    lax.fori_loop(0, CONV_CHUNKS, project, 0)

    @pl.when(place < length - 1)
    def _():
        hop(place, 0).wait_send()

    @pl.when(place > 0)
    def _():
        hop(place, 1).wait_send()

    def finish_line(m, carry):
        route(m).wait_send()
        origin = on_line(place, m, length)

        @pl.when((origin < place) & (place < length - 1))
        def _():
            hop(origin, 0).wait_send()

        @pl.when((origin > place) & (place > 0))
        def _():
            hop(origin, 1).wait_send()

        cross(m).wait_send()
        return carry

    cross(0).wait_send()
    cross_side().wait_send()
    lax.fori_loop(1, length, finish_line, 0)
    edge(0).wait_send()
    edge(1).wait_send()

    def finish_conv(c, carry):
        for number in range(3):
            conv_share(c, number).wait_send()
        if projected is not None:
            for q in range(quarters):
                kept_out(c, q).wait()
        return carry

    lax.fori_loop(0, CONV_CHUNKS, finish_conv, 0)

    def finish_units(p, carry):
        for number in range(3):
            units(p, number).wait_send()
        return carry

    lax.fori_loop(0, count, finish_units, 0)

    def fetch(origin):
        spot = landed.at[origin, :, :, pl.ds(width - features, features)]
        return pltpu.make_async_copy(returned.at[origin], spot, fetch_sem.at[origin])

    kept().wait()
    fetch(group).start()

    def fetch_next(m, carry):
        origin = on_line(place, m // 2, length) * 2 + (across + m) % 2
        back_from(origin).wait_recv()
        fetch(origin).start()
        return carry

    lax.fori_loop(1, count, fetch_next, 0)

    def wait_fetch(m, carry):
        fetch(m).wait()
        return carry

    lax.fori_loop(0, count, wait_fetch, 0)

    def kept_combined(q):
        source = normed.at[:, pl.ds(pl.multiple_of(q * features, LANES), features)]
        rows = pl.ds(q * MOE_DEV, MOE_DEV)
        return pltpu.make_async_copy(source, combined.at[rows], combine_kept.at[q])

    def combine(q, carry):
        start = pl.multiple_of(q * 2 * slots, LANES)
        values = landed[:, q, :, width - features : width].reshape(slots, features)
        gates = expert_gate.at[q]
        scale = group_gate[q] / (gates[0:1, :] + gates[1:2, :])
        total = jnp.zeros((MOE_DEV, features), jnp.float32)
        for k in range(TOP):
            share = jnp.broadcast_to(gates[k : k + 1, :] * scale, (MOE_DEV, MOE_DEV))
            columns = pl.ds(pl.multiple_of(start + k * slots, LANES), slots)
            part = jnp.dot(spare[:, columns], values, preferred_element_type=jnp.float32)
            total = total + jnp.transpose(share)[:, 0:1] * part
        columns = pl.ds(pl.multiple_of(q * features, LANES), features)
        normed[:, columns] = total.astype(jnp.bfloat16)
        kept_combined(q).start()
        return carry

    lax.fori_loop(0, quarters, combine, 0)

    def finish_combined(q, carry):
        kept_combined(q).wait()
        return carry

    lax.fori_loop(0, quarters, finish_combined, 0)

    def finish(m, carry):
        back(m).wait_send()
        return carry

    lax.fori_loop(1, count, finish, 0)


def fused(
    tokens,
    expert_gain,
    routes,
    gate_weight,
    up_weight,
    down_weight,
    conv_value,
    conv_gate,
    conv_taps,
    conv_gain,
    conv_bias,
    projection,
    group_gate,
    expert_gate,
    count,
):
    width = tokens.shape[1]
    quarters = tokens.shape[0] // MOE_DEV
    local, units, features = gate_weight.shape[0], gate_weight.shape[2], down_weight.shape[2]
    size = local * CAP
    length = count // 2
    positions, channels = conv_value.shape
    rows_per = positions // CONV_CHUNKS
    reach = conv_taps.shape[0] - 1
    border = -(-reach // 16) * 16
    rows = count * quarters * size
    dma = pltpu.SemaphoreType.DMA
    anywhere = pl.BlockSpec(memory_space=pl.ANY)
    inside = pl.BlockSpec(memory_space=pltpu.VMEM)
    inside_too = (
        rows_per == size
        and CONV_CHUNKS <= count
        and channels + 2 * features <= width
        and features == local * units
    )

    def kernel(*refs):
        if inside_too:
            return fused_kernel(count, reach, *refs)
        return fused_kernel(count, reach, *refs[:17], None, *refs[17:])

    out_shape = (
        jax.ShapeDtypeStruct((count, quarters, size, features), jnp.bfloat16),
        jax.ShapeDtypeStruct((quarters, positions, channels), jnp.bfloat16),
        jax.ShapeDtypeStruct((quarters * MOE_DEV, features), jnp.bfloat16),
        jax.ShapeDtypeStruct((quarters * positions, features), jnp.bfloat16),
    )
    outputs = 3 + inside_too
    results = pl.pallas_call(
        kernel,
        out_shape=out_shape[:outputs],
        in_specs=[
            anywhere,
            inside,
            inside,
            anywhere,
            anywhere,
            anywhere,
            anywhere,
            anywhere,
            inside,
            inside,
            inside,
            anywhere,
            inside,
            inside,
        ],
        out_specs=(anywhere,) * outputs,
        scratch_shapes=[
            pltpu.VMEM((length, MOE_DEV, width), jnp.bfloat16),
            pltpu.VMEM((length,) + routes.shape[1:], jnp.int32),
            pltpu.VMEM((MOE_DEV, max(width, 2 * rows)), jnp.bfloat16),
            pltpu.VMEM((MOE_DEV, max(width, quarters * features)), jnp.bfloat16),
            pltpu.VMEM((length + 1, size, width), jnp.bfloat16),
            pltpu.VMEM((count, quarters, size, width), jnp.bfloat16),
            pltpu.VMEM(gate_weight.shape, jnp.bfloat16),
            pltpu.VMEM(up_weight.shape, jnp.bfloat16),
            pltpu.VMEM(down_weight.shape, jnp.bfloat16),
            pltpu.VMEM((count, quarters, quarters, size, units), jnp.bfloat16),
            pltpu.VMEM((count, quarters, size, features), jnp.bfloat16),
            pltpu.VMEM((2, rows_per, channels), jnp.bfloat16),
            pltpu.VMEM((2, rows_per, channels), jnp.bfloat16),
            pltpu.VMEM((2, border, channels), jnp.bfloat16),
            pltpu.VMEM((channels // LANES, border + rows_per, LANES), jnp.float32),
            pltpu.VMEM((channels // LANES, rows_per, LANES), jnp.float32),
            pltpu.VMEM((CONV_CHUNKS, rows_per, channels), jnp.bfloat16),
            dma((6,)),
            dma((2, 2)),
            dma((2,)),
            dma((2,)),
            dma((length,)),
            dma((length,)),
            dma((length, 2)),
            dma((length,)),
            dma((length + 1,)),
            dma((length + 1,)),
            dma((count,)),
            dma((count,)),
            dma((count, 2)),
            dma((count, 2)),
            dma((count, 3)),
            dma((count, 3)),
            dma((count,)),
            dma((count,)),
            dma((CONV_CHUNKS,)),
            dma((CONV_CHUNKS, 3)),
            dma((CONV_CHUNKS, 3)),
            dma((CONV_CHUNKS + 1, max(quarters, features // units))),
            dma((CONV_CHUNKS, quarters)),
            dma((count,)),
            dma((quarters,)),
        ],
        compiler_params=pltpu.CompilerParams(
            collective_id=0, has_side_effects=True, vmem_limit_bytes=67_043_328
        ),
        cost_estimate=pl.CostEstimate(
            flops=40 * rows * width * units, bytes_accessed=250_000_000, transcendentals=0
        ),
    )(
        tokens,
        expert_gain,
        routes,
        gate_weight,
        up_weight,
        down_weight,
        conv_value,
        conv_gate,
        conv_taps,
        conv_gain,
        conv_bias,
        projection,
        group_gate,
        expert_gate,
    )
    if inside_too:
        return results[2], results[3]
    projected = jnp.dot(
        results[1].reshape(-1, channels), projection, preferred_element_type=jnp.float32
    )
    return results[2], projected.astype(jnp.bfloat16)


def on_device(
    conv_value,
    conv_gate,
    conv_taps,
    conv_gain,
    conv_bias,
    conv_projection,
    expert_input,
    expert_gain,
    route_experts,
    group_gate,
    expert_gate,
    gate_weight,
    up_weight,
    down_weight,
):
    count = lax.axis_size("ep")
    quarters = expert_input.shape[0] // MOE_DEV

    def by_lanes(values):
        return jnp.swapaxes(values.reshape(quarters, MOE_DEV, -1), 1, 2)

    expert_out, conv_out = fused(
        expert_input,
        expert_gain[None],
        by_lanes(route_experts),
        gate_weight,
        up_weight,
        down_weight,
        conv_value,
        conv_gate,
        conv_taps,
        conv_gain[None],
        conv_bias[None],
        conv_projection,
        group_gate.reshape(quarters, 1, MOE_DEV),
        by_lanes(expert_gate),
        count,
    )
    return (conv_out, expert_out)


def solution(mesh):
    return jax.shard_map(
        on_device,
        mesh=mesh,
        in_specs=(
            P(("ep", "tp"), None),
            P(("ep", "tp"), None),
            P(),
            P(),
            P(),
            P(None, "tp"),
            P("ep", None),
            P(),
            P("ep", None),
            P("ep"),
            P("ep", None),
            P("ep", None, "tp"),
            P("ep", None, "tp"),
            P("ep", None, "tp"),
        ),
        out_specs=(P("ep", "tp"), P("ep", "tp")),
        check_vma=False,
    )
```
